32 devices in a mesh: sp: 8 (over z, y), tp: 4 (over x, core).
Axes of the slice: x: 2, y: 2, z: 4, core: 2. Of those that a mesh axis runs over, the one named last changes fastest.
Arguments:
- hidden: bfloat16 [6144, 2048], P(('sp', 'tp')), may hold values from -6 to 6
- norm_gain: float32 [2, 2048], replicated, may hold values from 0.1 to 1.9
- w_value: bfloat16 [2, 2048, 2048], P(None, 'sp', 'tp'), may hold values from -0.125 to 0.125
- w_gate: bfloat16 [2, 2048, 2048], P(None, 'sp', 'tp'), may hold values from -0.125 to 0.125
- conv_weight: float32 [2, 31, 2048], P(None, None, 'tp'), may hold values from -3 to 3
- conv_bias: float32 [2, 2048], P(None, 'tp'), may hold values from -3 to 3
- chan_gain: float32 [2, 2048], P(None, 'tp'), may hold values from 0.1 to 1.9
- chan_shift: float32 [2, 2048], P(None, 'tp'), may hold values from -3 to 3
- w_out: bfloat16 [2, 2048, 2048], P(None, 'tp', 'sp'), may hold values from -0.125 to 0.125
Outputs:
- result: bfloat16 [6144, 2048], P(('sp', 'tp'))
The draws below stay inside these ranges and needn't reach their ends.
All inputs are finite; a program needn't handle non-finite values.
Results may differ from the reference program's by a relative error of at most 0.015.
Values may be sent and summed in bfloat16 or wider, within the bound.
A program may use at most 64 MiB of HBM per device.

```python
import jax
import jax.numpy as jnp
from jax import lax

D = 2048
C = 2048
K = 31
LAYERS = 2
TOKENS = 6144
N_TP = 4


def draw_conv_weight(key, part):
    key_base = jax.random.fold_in(key, 11)
    key_perm = jax.random.fold_in(key, 12)
    base = jnp.clip(jax.random.normal(key_base, (LAYERS, K, C), jnp.float32), -4.0, 4.0)
    ladder = 0.3 * 10.0 ** (jnp.arange(8, dtype=jnp.float32) / 7.0)
    levels = jnp.stack([ladder[jax.random.permutation(jax.random.fold_in(key_perm, layer), 8)] for layer in range(LAYERS)])
    scales = jnp.repeat(levels, C // 8, axis=1)
    return base * K ** (-0.5) * scales[:, None, :]


def shard_levels(rng, dims, pieces, low, largest):
    level = 1.0
    for axis_at, shards_of in pieces:
        heights = jax.random.uniform(jax.random.fold_in(jax.random.fold_in(rng, 6), axis_at), (shards_of,), jnp.float32, low / len(pieces), largest / len(pieces))
        level = level * jnp.repeat(jnp.exp(heights), dims[axis_at] // shards_of).reshape((-1,) + (1,) * (len(dims) - 1 - axis_at))
    return level


def centred(own_key, shape, scale, reach, split=(), kind=jnp.bfloat16):
    level = shard_levels(own_key, shape, split, -0.22, 0.18) if split else 1.0
    drawn = jax.random.normal(own_key, shape, jnp.float32) * scale * level
    return jnp.minimum(jnp.maximum(drawn, -reach), reach).astype(kind)


def setup_inputs(seed: int = 0) -> dict:
    arg_keys = jax.random.split(jax.random.key(seed), 10)
    hidden = centred(arg_keys[0], (TOKENS, D), 1.0, 6.0, ((0, 32),))
    norm_gain = jnp.clip(1.0 + 0.18 * jax.random.normal(arg_keys[1], (LAYERS, D), jnp.float32), 0.1, 1.9)
    w_value = centred(arg_keys[2], (LAYERS, D, C), D ** -0.5, 0.125, ((1, 8), (2, 4)))
    w_gate = centred(arg_keys[3], (LAYERS, D, C), D ** -0.5, 0.125, ((1, 8), (2, 4)))
    conv_weight = draw_conv_weight(jax.random.fold_in(arg_keys[9], 71), 0)
    conv_bias = centred(arg_keys[5], (LAYERS, C), 0.5, 3.0, ((1, 4),), jnp.float32)
    chan_gain = jnp.clip(1.0 + 0.18 * jax.random.normal(arg_keys[6], (LAYERS, C), jnp.float32), 0.1, 1.9)
    chan_shift = centred(arg_keys[7], (LAYERS, C), 0.5, 3.0, ((1, 4),), jnp.float32)
    w_out = centred(arg_keys[8], (LAYERS, C, D), C ** -0.5, 0.125, ((1, 4), (2, 8)))
    return dict(hidden=hidden, norm_gain=norm_gain, w_value=w_value, w_gate=w_gate, conv_weight=conv_weight, conv_bias=conv_bias, chan_gain=chan_gain, chan_shift=chan_shift, w_out=w_out)


EPS = 1e-06

def reference(hidden, norm_gain, w_value, w_gate, conv_weight, conv_bias, chan_gain, chan_shift, w_out):
    state = hidden
    width = C // N_TP
    for layer in range(LAYERS):
        xf = state.astype(jnp.float32)
        scale = lax.rsqrt(lax.optimization_barrier(jnp.mean(xf * xf, axis=1, keepdims=True)) + EPS)
        normed = (xf * scale * norm_gain[layer][None, :]).astype(jnp.bfloat16)
        lin = jnp.dot(normed, w_value[layer], preferred_element_type=jnp.float32)
        gate = jnp.dot(normed, w_gate[layer], preferred_element_type=jnp.float32)
        glu = (lin * jax.nn.sigmoid(gate)).astype(jnp.bfloat16)
        padded = jnp.concatenate([jnp.zeros((K - 1, C), jnp.bfloat16), glu], axis=0).astype(jnp.float32)
        mixed = jnp.zeros((TOKENS, C), jnp.float32) + conv_bias[layer][None, :]
        for tap in range(K):
            mixed = mixed + conv_weight[layer, tap][None, :] * padded[tap:tap + TOKENS]
        mean = lax.optimization_barrier(jnp.mean(mixed, axis=1, keepdims=True))
        msq = lax.optimization_barrier(jnp.mean(mixed * mixed, axis=1, keepdims=True))
        var = msq - mean * mean
        act = jax.nn.silu((mixed - mean) * lax.rsqrt(var + EPS) * chan_gain[layer][None, :] + chan_shift[layer][None, :]).astype(jnp.bfloat16)
        update = jnp.zeros((TOKENS, D), jnp.float32)
        for block in range(N_TP):
            part = jnp.dot(act[:, block * width:(block + 1) * width], w_out[layer, block * width:(block + 1) * width, :], preferred_element_type=jnp.float32)
            part = lax.optimization_barrier(part.astype(jnp.bfloat16))
            update = update + part.astype(jnp.float32)
        state = (xf + update).astype(jnp.bfloat16)
    return state
```

```python
import functools

import jax
import jax.numpy as jnp
from jax import lax
from jax.experimental import pallas as pl
from jax.experimental.pallas import tpu as pltpu
from jax.sharding import PartitionSpec as P

EPS = 1e-06
F32 = jnp.float32
BF16 = jnp.bfloat16
MESH = pl.DeviceIdType.MESH
RT = 128
HALO = 32
LANES = 128


def dot(a, b):
    return jnp.dot(a, b, preferred_element_type=F32)


def kernel(Z, Y, X, h_ref, gain_ref, wv_ref, wg_ref, cw_ref, cb_ref, cg_ref, cs_ref, wo_ref, o_ref,
           WV, WG, WO, TOK, PT, PI, PX, RX, GLF, HB, MIX, S1, S2, ST, ACT, HS,
           w_rs, wz_ss, wz2_ss, wy_ss, t_ss, t_rs, h_ss, h_rs, s_ss, s_rs, d_ss, d_rs, x_ss, x_rs):
    L = gain_ref.shape[0]
    own_rows, D = h_ref.shape
    rows = wv_ref.shape[1]
    C = wv_ref.shape[2]
    NT = 2 * X
    M = own_rows * NT
    taps = cw_ref.shape[1]
    wcols = wo_ref.shape[2]
    s = lax.axis_index("sp")
    t = lax.axis_index("tp")
    z, y = s // Y, lax.rem(s, Y)
    x, c = t // 2, lax.rem(t, 2)
    units = [(l, k) for l in range(L) for k in range(3)]
    U = len(units)
    scheme_a = [u == 2 for u in range(U)]

    def wrap(v, n):
        return lax.rem(v + n, n)

    def sdev(zz, yy):
        return (zz * Y + yy, t)

    def tdev(xx, cc):
        return (s, xx * 2 + cc)

    partner = tdev(x, 1 - c)
    nxt = (wrap(s + 1, Z * Y), t)
    prev = (wrap(s - 1, Z * Y), t)
    zp = sdev(wrap(z + 1, Z), y)
    zm = sdev(wrap(z - 1, Z), y)
    has_p, has_m = z + 1 < Z, z >= 1

    bar = pltpu.get_barrier_semaphore()

    def greet(dev):
        pl.semaphore_signal(bar, inc=1, device_id=dev, device_id_type=MESH)

    count = 0
    for yo in range(1, Y):
        greet(sdev(z, wrap(y + yo, Y)))
        count += 1
    for o in range(1, NT):
        greet((s, wrap(t + o, NT)))
        count += 1

    @pl.when(has_p)
    def _():
        greet(zp)

    @pl.when(has_m)
    def _():
        greet(zm)

    @pl.when(s + 1 < Z * Y)
    def _():
        greet(nxt)

    @pl.when(s >= 1)
    def _():
        greet(prev)

    peers = count + sum(cond.astype(jnp.int32) for cond in (has_p, has_m, s + 1 < Z * Y, s >= 1))
    pl.semaphore_wait(bar, peers)

    def piece(u, src):
        l, k = units[u]
        if k == 2:
            return WO.at[l, src]
        w = WV if k == 0 else WG
        return w.at[l, pl.ds(pl.multiple_of(src * rows, rows), rows), :]

    def own_piece(u):
        l, k = units[u]
        return (wv_ref, wg_ref, wo_ref)[k].at[l]

    def wcopy(u, src, dev, ssem, first):
        return pltpu.make_async_remote_copy(
            src_ref=own_piece(u) if first else piece(u, src), dst_ref=piece(u, src),
            send_sem=ssem, recv_sem=w_rs.at[u, src], device_id=dev, device_id_type=MESH)

    pending = []

    def go(cond, make):
        def _():
            make().start()
        if cond is None:
            _()
        else:
            pl.when(cond)(_)
        pending.append((cond, make))

    def drain():
        for cond, make in pending:
            def _(make=make):
                make().wait_send()
            if cond is None:
                _()
            else:
                pl.when(cond)(_)
        pending.clear()

    def wait_w(u, src):
        wcopy(u, src, zp, wz_ss.at[u, src], False).wait_recv()

    def send_own(u):
        go(has_p, lambda: wcopy(u, s, zp, wz_ss.at[u, s], True))
        go(has_m, lambda: wcopy(u, s, zm, wz2_ss.at[u, y], True))
        for yo in range(1, Y):
            go(None, lambda yo=yo: wcopy(u, s, sdev(z, wrap(y + yo, Y)), wy_ss.at[u, z, yo - 1], True))
        l, k = units[u]
        if k == 2:
            WO[l, s] = wo_ref[l]
        else:
            w, r = ((WV, wv_ref), (WG, wg_ref))[k]
            w[l, pl.ds(pl.multiple_of(s * rows, rows), rows), :] = r[l]

    def ev_p(u):
        for yo in range(1, Y):
            yy = wrap(y + yo, Y)
            src = z * Y + yy
            wait_w(u, src)
            go(has_p, lambda src=src: wcopy(u, src, zp, wz_ss.at[u, src], False))
            go(has_m, lambda src=src, yy=yy: wcopy(u, src, zm, wz2_ss.at[u, yy], False))

    def ev_d(u, k):
        for sgn in (1, -1):
            zs = wrap(z - sgn * k, Z)
            valid = z >= k if sgn == 1 else z + k < Z
            fwd = jnp.logical_and(valid, has_p if sgn == 1 else has_m)
            dev = zp if sgn == 1 else zm
            src = zs * Y + y

            @pl.when(valid)
            def _():
                wait_w(u, src)
            go(fwd, lambda src=src, dev=dev: wcopy(u, src, dev, wz_ss.at[u, src], False))
            for yo in range(1, Y):
                yy = wrap(y + yo, Y)
                if scheme_a[u]:
                    src2 = zs * Y + yy

                    @pl.when(valid)
                    def _():
                        wait_w(u, src2)
                    go(fwd, lambda src2=src2, dev=dev: wcopy(u, src2, dev, wz_ss.at[u, src2], False))
                else:
                    go(valid, lambda src=src, yy=yy, yo=yo, zs=zs: wcopy(
                        u, src, sdev(z, yy), wy_ss.at[u, zs, yo - 1], False))

    def zorder(j):
        return jnp.where(z < Z // 2, wrap(z + j, Z), wrap(z - j, Z))

    def fin(u):
        if not scheme_a[u]:
            for j in range(Z):
                for yo in range(1, Y):
                    wait_w(u, zorder(j) * Y + wrap(y + yo, Y))

    def tcopy(l, slot, dev, i):
        ref = TOK.at[l, pl.ds(pl.multiple_of(slot * own_rows, own_rows), own_rows), :]
        return pltpu.make_async_remote_copy(
            src_ref=ref, dst_ref=ref, send_sem=t_ss.at[l, i], recv_sem=t_rs.at[l, slot],
            device_id=dev, device_id_type=MESH)

    NR = own_rows // 4 if own_rows % 64 == 0 else own_rows // 2

    def norm_send(l):
        def nb(i, _):
            r = pl.ds(pl.multiple_of(i * NR, NR), NR)
            xf = (h_ref if l == 0 else HS)[r, :].astype(F32)
            scale = lax.rsqrt(jnp.mean(xf * xf, axis=1, keepdims=True) + EPS)
            TOK[l, pl.ds(pl.multiple_of(t * own_rows + i * NR, NR), NR), :] = (
                xf * scale * gain_ref[l, :][None, :]).astype(BF16)
            return 0
        lax.fori_loop(0, own_rows // NR, nb, 0)
        for o in range(1, X):
            go(None, lambda o=o: tcopy(l, t, tdev(wrap(x + o, X), c), o - 1))
        go(None, lambda: tcopy(l, t, partner, X - 1))

    def tok_relay(l):
        for o in range(1, X):
            slot = wrap(x - o, X) * 2 + c
            tcopy(l, slot, partner, 0).wait_recv()
            go(None, lambda o=o, slot=slot: tcopy(l, slot, partner, X - 1 + o))

    def tok_fin(l):
        for o in range(X):
            tcopy(l, wrap(x - o, X) * 2 + 1 - c, partner, 0).wait_recv()

    NC = C // LANES

    def project(l):
        def mb(i, _):
            r = pl.ds(pl.multiple_of(i * RT, RT), RT)
            a = TOK[l, r, :]
            lin = dot(a, WV[l])
            gate = dot(a, WG[l])
            glu = (lin * jax.nn.sigmoid(gate)).astype(BF16).astype(F32)
            for n in range(NC):
                GLF[n, pl.ds(pl.multiple_of(HALO + i * RT, 8), RT), :] = glu[:, n * LANES:(n + 1) * LANES]
            return 0
        lax.fori_loop(0, M // RT, mb, 0)
        for n in range(NC):
            HB[l, 0, :, n * LANES:(n + 1) * LANES] = GLF[n, M:M + HALO, :].astype(BF16)
        go(s + 1 < Z * Y, lambda: hcopy(l))

    def hcopy(l):
        return pltpu.make_async_remote_copy(
            src_ref=HB.at[l, 0], dst_ref=HB.at[l, 1], send_sem=h_ss.at[l], recv_sem=h_rs.at[l],
            device_id=nxt, device_id_type=MESH)

    def halo_fin(l):
        @pl.when(s >= 1)
        def _():
            hcopy(l).wait_recv()
            for n in range(NC):
                GLF[n, 0:HALO, :] = HB[l, 1, :, n * LANES:(n + 1) * LANES].astype(F32)

        @pl.when(s == 0)
        def _():
            for n in range(NC):
                GLF[n, 0:HALO, :] = jnp.zeros((HALO, LANES), F32)

    CT = 64

    def conv_tile(l, i):
        first = HALO - (taps - 1)
        s1 = jnp.zeros((CT, LANES), F32)
        s2 = jnp.zeros((CT, LANES), F32)
        base = pl.multiple_of(i * CT, CT)
        for n in range(NC):
            lanes = slice(n * LANES, (n + 1) * LANES)
            acc = jnp.zeros((CT, LANES), F32) + cb_ref[l:l + 1, lanes]
            for tap in range(taps):
                acc = acc + cw_ref[l, tap:tap + 1, lanes] * GLF[n, pl.ds(base + first + tap, CT), :]
            MIX[pl.ds(base, CT), lanes] = acc
            s1 = s1 + acc
            s2 = s2 + acc * acc
        S1[pl.ds(base, CT), :] = s1
        S2[pl.ds(base, CT), :] = s2

    def conv(l, lo, hi):
        def cbody(i, _):
            conv_tile(l, i)
            return 0
        lax.fori_loop(lo, hi, cbody, 0)

    def scopy(l, o):
        return pltpu.make_async_remote_copy(
            src_ref=ST.at[l, 0], dst_ref=ST.at[l, o], send_sem=s_ss.at[l, o - 1], recv_sem=s_rs.at[l, o - 1],
            device_id=(s, wrap(t + o, NT)), device_id_type=MESH)

    def stats_send(l):
        for i in range(M // RT):
            r = slice(i * RT, (i + 1) * RT)
            a = jnp.sum(jnp.transpose(S1[r, :]), axis=0, keepdims=True)
            b = jnp.sum(jnp.transpose(S2[r, :]), axis=0, keepdims=True)
            ST[l, 0, 0:1, r] = a
            ST[l, 0, 1:2, r] = b
        ST[l, 0, 2:8, :] = jnp.zeros((6, M), F32)
        for o in range(1, NT):
            go(None, lambda o=o: scopy(l, o))

    def activate(l):
        for o in range(1, NT):
            scopy(l, o).wait_recv()
        for i in range(M // RT):
            r = slice(i * RT, (i + 1) * RT)
            tot = ST[l, 0, :, r]
            for o in range(1, NT):
                tot = tot + ST[l, o, :, r]
            tot = tot / (C * NT)
            mean = tot[0:1, :]
            var = tot[1:2, :] - mean * mean
            inv = lax.rsqrt(var + EPS)
            mb = jnp.transpose(jnp.broadcast_to(mean, (LANES, RT)))
            ib = jnp.transpose(jnp.broadcast_to(inv, (LANES, RT)))
            S1[r, :] = mb
            S2[r, :] = ib

        def ab(i, _):
            r = pl.ds(pl.multiple_of(i * CT, CT), CT)
            mb, ib = S1[r, :], S2[r, :]
            for n in range(NC):
                lanes = slice(n * LANES, (n + 1) * LANES)
                v = (MIX[r, lanes] - mb) * ib * cg_ref[l:l + 1, lanes] + cs_ref[l:l + 1, lanes]
                ACT[r, lanes] = (v / (1.0 + jnp.exp(-v))).astype(BF16)
            return 0
        lax.fori_loop(0, M // CT, ab, 0)

    def dcopy(l, src):
        return pltpu.make_async_remote_copy(
            src_ref=PT.at[l, src, pl.ds(X, X)], dst_ref=PI.at[l, src],
            send_sem=d_ss.at[l, src], recv_sem=d_rs.at[l, src], device_id=partner, device_id_type=MESH)

    def xcopy(l, src, o):
        return pltpu.make_async_remote_copy(
            src_ref=PX.at[l, src, o - 1], dst_ref=RX.at[l, src, o - 1],
            send_sem=x_ss.at[l, src, o - 1], recv_sem=x_rs.at[l, src, o - 1],
            device_id=tdev(wrap(x + o, X), c), device_id_type=MESH)

    def chunk(l, src):
        def qb(q, _):
            off, other = lax.rem(q, X), q // X
            cc = jnp.where(other == 0, c, 1 - c)
            td = lax.rem(x + off, X) * 2 + cc
            a = ACT[pl.ds(pl.multiple_of(td * own_rows, own_rows), own_rows), :]
            PT[l, src, q] = dot(a, WO[l, src]).astype(BF16)
            return 0
        lax.fori_loop(0, 2 * X, qb, 0)
        go(None, lambda: dcopy(l, src))

    def chunk_x(l, src):
        dcopy(l, src).wait_recv()
        for o in range(1, X):
            PX[l, src, o - 1] = (PT[l, src, o].astype(F32) + PI[l, src, o].astype(F32)).astype(BF16)
            go(None, lambda o=o: xcopy(l, src, o))

    def finish(l):
        last = l == L - 1
        for src in range(Z * Y):
            upd = PT[l, src, 0].astype(F32) + PI[l, src, 0].astype(F32)
            for o in range(1, X):
                xcopy(l, src, o).wait_recv()
                upd = upd + RX[l, src, o - 1].astype(F32)
            cols = slice(src * wcols, (src + 1) * wcols)
            old = (h_ref if l == 0 else HS)[:, cols].astype(F32)
            (o_ref if last else HS)[:, cols] = (old + upd).astype(BF16)

    state = {"prev": None}

    def do_chunk(l, j, yo):
        src = zorder(j) * Y + wrap(y + yo, Y)
        chunk(l, src)
        if state["prev"] is not None:
            chunk_x(*state["prev"])
        state["prev"] = (l, src)

    def flush_chunk():
        chunk_x(*state["prev"])
        state["prev"] = None

    send_own(0)
    send_own(1)
    norm_send(0)
    for l in range(L):
        v, g, w = 3 * l, 3 * l + 1, 3 * l + 2
        more = l + 1 < L
        if l == 0:
            ev_d(v, 1)
            for k in range(2, Z):
                ev_d(v, k)
            send_own(w)
            tok_relay(l)
            ev_d(g, 1)
            for k in range(2, Z):
                ev_d(g, k)
            if scheme_a[w]:
                ev_p(w)
            if more:
                send_own(v + 3)
            ev_d(w, 1)
        fin(v)
        fin(g)
        tok_fin(l)
        project(l)
        if l > 0:
            for k in range(1, Z - 1):
                ev_d(w, k)
        conv(l, 1, M // CT // 2)
        if l == 0 and Z > 2:
            ev_d(w, 2)
        conv(l, M // CT // 2, M // CT)
        halo_fin(l)
        conv(l, 0, 1)
        stats_send(l)
        if more:
            for k in range(3, Z):
                ev_d(w, k)
            send_own(g + 3)
            ev_d(v + 3, 1)
        activate(l)
        if more:
            do_chunk(l, 0, 0)
            ev_d(v + 3, 2)
            send_own(w + 3)
        else:
            do_chunk(l, 0, 0)
            ev_d(w, Z - 1)
        for j in range(1, Z):
            do_chunk(l, j, 0)
        if more:
            for k in range(3, Z):
                ev_d(v + 3, k)
        for j in range(Z):
            for yo in range(1, Y):
                if not scheme_a[w]:
                    wait_w(w, zorder(j) * Y + wrap(y + yo, Y))
                do_chunk(l, j, yo)
        flush_chunk()
        if more:
            ev_d(g + 3, 1)
        finish(l)
        if more:
            norm_send(l + 1)
            for k in range(2, Z):
                ev_d(g + 3, k)
            tok_relay(l + 1)
    drain()


def solution(mesh):
    sp, tp = mesh.shape["sp"], mesh.shape["tp"]
    Y = 1
    while (2 * Y) * (2 * Y) <= sp:
        Y *= 2
    Z, X = sp // Y, tp // 2

    def body(*args):
        hidden, norm_gain, w_value, w_gate, conv_weight, conv_bias, chan_gain, chan_shift, w_out = args
        own_rows, D = hidden.shape
        L, rows, C = w_value.shape
        wcols = w_out.shape[2]
        M = own_rows * tp
        U = 3 * L
        vm = pltpu.VMEM
        dma = pltpu.SemaphoreType.DMA
        nx = max(X - 1, 1)
        return pl.pallas_call(
            functools.partial(kernel, Z, Y, X),
            out_shape=jax.ShapeDtypeStruct((own_rows, D), BF16),
            in_specs=[pl.BlockSpec(memory_space=pltpu.VMEM)] * 9,
            out_specs=pl.BlockSpec(memory_space=pltpu.VMEM),
            scratch_shapes=[
                vm((L, sp * rows, C), BF16), vm((L, sp * rows, C), BF16), vm((L, sp, C, wcols), BF16),
                vm((L, M, D), BF16),
                vm((L, sp, 2 * X, own_rows, wcols), BF16), vm((L, sp, X, own_rows, wcols), BF16),
                vm((L, sp, nx, own_rows, wcols), BF16), vm((L, sp, nx, own_rows, wcols), BF16),
                vm((C // LANES, HALO + M, LANES), F32), vm((L, 2, HALO, C), BF16),
                vm((M, C), F32), vm((M, LANES), F32), vm((M, LANES), F32),
                vm((L, tp, 8, M), F32), vm((M, C), BF16), vm((own_rows, D), BF16),
                dma((U, sp)), dma((U, sp)), dma((U, Y)), dma((U, Z, max(Y - 1, 1))),
                dma((L, 2 * X)), dma((L, tp)), dma((L,)), dma((L,)), dma((L, tp - 1)), dma((L, tp - 1)),
                dma((L, sp)), dma((L, sp)), dma((L, sp, nx)), dma((L, sp, nx)),
            ],
            compiler_params=pltpu.CompilerParams(
                collective_id=0, has_side_effects=True, vmem_limit_bytes=65000 * 1024),
        )(*args)

    placed = (
        P(("sp", "tp"), None), P(), P(None, "sp", "tp"), P(None, "sp", "tp"), P(None, None, "tp"),
        P(None, "tp"), P(None, "tp"), P(None, "tp"), P(None, "tp", "sp"),
    )
    return jax.shard_map(
        body, mesh=mesh, in_specs=placed, out_specs=P(("sp", "tp"), None), check_vma=False)
```

```python
import functools

import jax
import jax.numpy as jnp
from jax import lax
from jax.experimental import pallas as pl
from jax.experimental.pallas import tpu as pltpu
from jax.sharding import PartitionSpec as P

EPS = 1e-06
F32 = jnp.float32
BF16 = jnp.bfloat16
MESH = pl.DeviceIdType.MESH
RT = 128
HALO = 32
LANES = 128


def dot(a, b):
    return jnp.dot(a, b, preferred_element_type=F32)


def kernel(Z, Y, X, h_ref, gain_ref, wv_ref, wg_ref, cw_ref, cb_ref, cg_ref, cs_ref, wo_ref, o_ref,
           WV, WG, WO, TOK, PT, PI, PX, RX, GLF, HB, MIX, S1, S2, ST, ACT, HS,
           w_rs, wz_ss, wz2_ss, wy_ss, t_ss, t_rs, h_ss, h_rs, s_ss, s_rs, d_ss, d_rs, x_ss, x_rs):
    L = gain_ref.shape[0]
    own_rows, D = h_ref.shape
    rows = wv_ref.shape[1]
    C = wv_ref.shape[2]
    NT = 2 * X
    M = own_rows * NT
    taps = cw_ref.shape[1]
    wcols = wo_ref.shape[2]
    s = lax.axis_index("sp")
    t = lax.axis_index("tp")
    z, y = s // Y, lax.rem(s, Y)
    x, c = t // 2, lax.rem(t, 2)
    units = [(l, k) for l in range(L) for k in range(3)]
    U = len(units)
    scheme_a = [u == 3 for u in range(U)]

    def wrap(v, n):
        return lax.rem(v + n, n)

    def sdev(zz, yy):
        return (zz * Y + yy, t)

    def tdev(xx, cc):
        return (s, xx * 2 + cc)

    partner = tdev(x, 1 - c)
    nxt = (wrap(s + 1, Z * Y), t)
    prev = (wrap(s - 1, Z * Y), t)
    zp = sdev(wrap(z + 1, Z), y)
    zm = sdev(wrap(z - 1, Z), y)
    has_p, has_m = z + 1 < Z, z >= 1

    bar = pltpu.get_barrier_semaphore()

    def greet(dev):
        pl.semaphore_signal(bar, inc=1, device_id=dev, device_id_type=MESH)

    count = 0
    for yo in range(1, Y):
        greet(sdev(z, wrap(y + yo, Y)))
        count += 1
    for o in range(1, NT):
        greet((s, wrap(t + o, NT)))
        count += 1

    @pl.when(has_p)
    def _():
        greet(zp)

    @pl.when(has_m)
    def _():
        greet(zm)

    @pl.when(s + 1 < Z * Y)
    def _():
        greet(nxt)

    @pl.when(s >= 1)
    def _():
        greet(prev)

    peers = count + sum(cond.astype(jnp.int32) for cond in (has_p, has_m, s + 1 < Z * Y, s >= 1))
    pl.semaphore_wait(bar, peers)

    def piece(u, src):
        l, k = units[u]
        if k == 2:
            return WO.at[l, src]
        w = WV if k == 0 else WG
        return w.at[l, pl.ds(pl.multiple_of(src * rows, rows), rows), :]

    def own_piece(u):
        l, k = units[u]
        return (wv_ref, wg_ref, wo_ref)[k].at[l]

    def wcopy(u, src, dev, ssem, first):
        return pltpu.make_async_remote_copy(
            src_ref=own_piece(u) if first else piece(u, src), dst_ref=piece(u, src),
            send_sem=ssem, recv_sem=w_rs.at[u, src], device_id=dev, device_id_type=MESH)

    pending = []

    def go(cond, make):
        def _():
            make().start()
        if cond is None:
            _()
        else:
            pl.when(cond)(_)
        pending.append((cond, make))

    def drain():
        for cond, make in pending:
            def _(make=make):
                make().wait_send()
            if cond is None:
                _()
            else:
                pl.when(cond)(_)
        pending.clear()

    def wait_w(u, src):
        wcopy(u, src, zp, wz_ss.at[u, src], False).wait_recv()

    def send_own(u):
        go(has_p, lambda: wcopy(u, s, zp, wz_ss.at[u, s], True))
        go(has_m, lambda: wcopy(u, s, zm, wz2_ss.at[u, y], True))
        for yo in range(1, Y):
            go(None, lambda yo=yo: wcopy(u, s, sdev(z, wrap(y + yo, Y)), wy_ss.at[u, z, yo - 1], True))
        l, k = units[u]
        if k == 2:
            WO[l, s] = wo_ref[l]
        else:
            w, r = ((WV, wv_ref), (WG, wg_ref))[k]
            w[l, pl.ds(pl.multiple_of(s * rows, rows), rows), :] = r[l]

    def ev_p(u):
        for yo in range(1, Y):
            yy = wrap(y + yo, Y)
            src = z * Y + yy
            wait_w(u, src)
            go(has_p, lambda src=src: wcopy(u, src, zp, wz_ss.at[u, src], False))
            go(has_m, lambda src=src, yy=yy: wcopy(u, src, zm, wz2_ss.at[u, yy], False))

    def ev_d(u, k):
        for sgn in (1, -1):
            zs = wrap(z - sgn * k, Z)
            valid = z >= k if sgn == 1 else z + k < Z
            fwd = jnp.logical_and(valid, has_p if sgn == 1 else has_m)
            dev = zp if sgn == 1 else zm
            src = zs * Y + y

            @pl.when(valid)
            def _():
                wait_w(u, src)
            go(fwd, lambda src=src, dev=dev: wcopy(u, src, dev, wz_ss.at[u, src], False))
            for yo in range(1, Y):
                yy = wrap(y + yo, Y)
                if scheme_a[u]:
                    src2 = zs * Y + yy

                    @pl.when(valid)
                    def _():
                        wait_w(u, src2)
                    go(fwd, lambda src2=src2, dev=dev: wcopy(u, src2, dev, wz_ss.at[u, src2], False))
                else:
                    go(valid, lambda src=src, yy=yy, yo=yo, zs=zs: wcopy(
                        u, src, sdev(z, yy), wy_ss.at[u, zs, yo - 1], False))

    def zorder(j):
        return jnp.where(z < Z // 2, wrap(z + j, Z), wrap(z - j, Z))

    def fin(u):
        if not scheme_a[u]:
            for j in range(Z):
                for yo in range(1, Y):
                    wait_w(u, zorder(j) * Y + wrap(y + yo, Y))

    def tcopy(l, slot, dev, i):
        ref = TOK.at[l, pl.ds(pl.multiple_of(slot * own_rows, own_rows), own_rows), :]
        return pltpu.make_async_remote_copy(
            src_ref=ref, dst_ref=ref, send_sem=t_ss.at[l, i], recv_sem=t_rs.at[l, slot],
            device_id=dev, device_id_type=MESH)

    NR = own_rows // 4 if own_rows % 64 == 0 else own_rows // 2

    def norm_send(l):
        def nb(i, _):
            r = pl.ds(pl.multiple_of(i * NR, NR), NR)
            xf = (h_ref if l == 0 else HS)[r, :].astype(F32)
            scale = lax.rsqrt(jnp.mean(xf * xf, axis=1, keepdims=True) + EPS)
            TOK[l, pl.ds(pl.multiple_of(t * own_rows + i * NR, NR), NR), :] = (
                xf * scale * gain_ref[l, :][None, :]).astype(BF16)
            return 0
        lax.fori_loop(0, own_rows // NR, nb, 0)
        for o in range(1, X):
            go(None, lambda o=o: tcopy(l, t, tdev(wrap(x + o, X), c), o - 1))
        go(None, lambda: tcopy(l, t, partner, X - 1))

    def tok_relay(l):
        for o in range(1, X):
            slot = wrap(x - o, X) * 2 + c
            tcopy(l, slot, partner, 0).wait_recv()
            go(None, lambda o=o, slot=slot: tcopy(l, slot, partner, X - 1 + o))

    def tok_fin(l):
        for o in range(X):
            tcopy(l, wrap(x - o, X) * 2 + 1 - c, partner, 0).wait_recv()

    NC = C // LANES

    def project(l):
        def mb(i, _):
            r = pl.ds(pl.multiple_of(i * RT, RT), RT)
            a = TOK[l, r, :]
            lin = dot(a, WV[l])
            gate = dot(a, WG[l])
            glu = (lin * jax.nn.sigmoid(gate)).astype(BF16).astype(F32)
            for n in range(NC):
                GLF[n, pl.ds(pl.multiple_of(HALO + i * RT, 8), RT), :] = glu[:, n * LANES:(n + 1) * LANES]
            return 0
        lax.fori_loop(0, M // RT, mb, 0)
        for n in range(NC):
            HB[l, 0, :, n * LANES:(n + 1) * LANES] = GLF[n, M:M + HALO, :].astype(BF16)
        go(s + 1 < Z * Y, lambda: hcopy(l))

    def hcopy(l):
        return pltpu.make_async_remote_copy(
            src_ref=HB.at[l, 0], dst_ref=HB.at[l, 1], send_sem=h_ss.at[l], recv_sem=h_rs.at[l],
            device_id=nxt, device_id_type=MESH)

    def halo_fin(l):
        @pl.when(s >= 1)
        def _():
            hcopy(l).wait_recv()
            for n in range(NC):
                GLF[n, 0:HALO, :] = HB[l, 1, :, n * LANES:(n + 1) * LANES].astype(F32)

        @pl.when(s == 0)
        def _():
            for n in range(NC):
                GLF[n, 0:HALO, :] = jnp.zeros((HALO, LANES), F32)

    CT = 64

    def conv_tile(l, i):
        first = HALO - (taps - 1)
        s1 = jnp.zeros((CT, LANES), F32)
        s2 = jnp.zeros((CT, LANES), F32)
        base = pl.multiple_of(i * CT, CT)
        for n in range(NC):
            lanes = slice(n * LANES, (n + 1) * LANES)
            acc = jnp.zeros((CT, LANES), F32) + cb_ref[l:l + 1, lanes]
            for tap in range(taps):
                acc = acc + cw_ref[l, tap:tap + 1, lanes] * GLF[n, pl.ds(base + first + tap, CT), :]
            MIX[pl.ds(base, CT), lanes] = acc
            s1 = s1 + acc
            s2 = s2 + acc * acc
        S1[pl.ds(base, CT), :] = s1
        S2[pl.ds(base, CT), :] = s2

    def conv(l, lo, hi):
        def cbody(i, _):
            conv_tile(l, i)
            return 0
        lax.fori_loop(lo, hi, cbody, 0)

    def scopy(l, o):
        return pltpu.make_async_remote_copy(
            src_ref=ST.at[l, 0], dst_ref=ST.at[l, o], send_sem=s_ss.at[l, o - 1], recv_sem=s_rs.at[l, o - 1],
            device_id=(s, wrap(t + o, NT)), device_id_type=MESH)

    def stats_send(l):
        for i in range(M // RT):
            r = slice(i * RT, (i + 1) * RT)
            a = jnp.sum(jnp.transpose(S1[r, :]), axis=0, keepdims=True)
            b = jnp.sum(jnp.transpose(S2[r, :]), axis=0, keepdims=True)
            ST[l, 0, 0:1, r] = a
            ST[l, 0, 1:2, r] = b
        ST[l, 0, 2:8, :] = jnp.zeros((6, M), F32)
        for o in range(1, NT):
            go(None, lambda o=o: scopy(l, o))

    def activate(l):
        for o in range(1, NT):
            scopy(l, o).wait_recv()
        for i in range(M // RT):
            r = slice(i * RT, (i + 1) * RT)
            tot = ST[l, 0, :, r]
            for o in range(1, NT):
                tot = tot + ST[l, o, :, r]
            tot = tot / (C * NT)
            mean = tot[0:1, :]
            var = tot[1:2, :] - mean * mean
            inv = lax.rsqrt(var + EPS)
            mb = jnp.transpose(jnp.broadcast_to(mean, (LANES, RT)))
            ib = jnp.transpose(jnp.broadcast_to(inv, (LANES, RT)))
            S1[r, :] = mb
            S2[r, :] = ib

        def ab(i, _):
            r = pl.ds(pl.multiple_of(i * CT, CT), CT)
            mb, ib = S1[r, :], S2[r, :]
            for n in range(NC):
                lanes = slice(n * LANES, (n + 1) * LANES)
                v = (MIX[r, lanes] - mb) * ib * cg_ref[l:l + 1, lanes] + cs_ref[l:l + 1, lanes]
                ACT[r, lanes] = (v / (1.0 + jnp.exp(-v))).astype(BF16)
            return 0
        lax.fori_loop(0, M // CT, ab, 0)

    def dcopy(l, src):
        return pltpu.make_async_remote_copy(
            src_ref=PT.at[l, src, pl.ds(X, X)], dst_ref=PI.at[l, src],
            send_sem=d_ss.at[l, src], recv_sem=d_rs.at[l, src], device_id=partner, device_id_type=MESH)

    def xcopy(l, src, o):
        return pltpu.make_async_remote_copy(
            src_ref=PX.at[l, src, o - 1], dst_ref=RX.at[l, src, o - 1],
            send_sem=x_ss.at[l, src, o - 1], recv_sem=x_rs.at[l, src, o - 1],
            device_id=tdev(wrap(x + o, X), c), device_id_type=MESH)

    def chunk(l, src):
        def qb(q, _):
            off, other = lax.rem(q, X), q // X
            cc = jnp.where(other == 0, c, 1 - c)
            td = lax.rem(x + off, X) * 2 + cc
            a = ACT[pl.ds(pl.multiple_of(td * own_rows, own_rows), own_rows), :]
            PT[l, src, q] = dot(a, WO[l, src]).astype(BF16)
            return 0
        lax.fori_loop(0, 2 * X, qb, 0)
        go(None, lambda: dcopy(l, src))

    def chunk_x(l, src):
        dcopy(l, src).wait_recv()
        for o in range(1, X):
            PX[l, src, o - 1] = (PT[l, src, o].astype(F32) + PI[l, src, o].astype(F32)).astype(BF16)
            go(None, lambda o=o: xcopy(l, src, o))

    def finish(l):
        last = l == L - 1
        for src in range(Z * Y):
            upd = PT[l, src, 0].astype(F32) + PI[l, src, 0].astype(F32)
            for o in range(1, X):
                xcopy(l, src, o).wait_recv()
                upd = upd + RX[l, src, o - 1].astype(F32)
            cols = slice(src * wcols, (src + 1) * wcols)
            old = (h_ref if l == 0 else HS)[:, cols].astype(F32)
            (o_ref if last else HS)[:, cols] = (old + upd).astype(BF16)

    state = {"prev": None}

    def do_chunk(l, j, yo):
        src = zorder(j) * Y + wrap(y + yo, Y)
        chunk(l, src)
        if state["prev"] is not None:
            chunk_x(*state["prev"])
        state["prev"] = (l, src)

    def flush_chunk():
        chunk_x(*state["prev"])
        state["prev"] = None

    def ev_rest(u, k0):
        for k in range(k0, Z):
            ev_d(u, k)

    send_own(0)
    send_own(1)
    norm_send(0)
    for l in range(L):
        v, g, w = 3 * l, 3 * l + 1, 3 * l + 2
        more = l + 1 < L
        if l == 0:
            ev_d(v, 1)
            ev_d(v, 2)
            send_own(w)
            ev_rest(v, 3)
            tok_relay(l)
            ev_d(g, 1)
            ev_d(g, 2)
            if more:
                send_own(v + 3)
            ev_rest(g, 3)
            ev_d(w, 1)
        fin(v)
        fin(g)
        tok_fin(l)
        project(l)
        if l == 0:
            ev_d(w, 2)
            if more:
                send_own(g + 3)
                if scheme_a[v + 3]:
                    ev_p(v + 3)
        conv(l, 1, M // CT // 2)
        if l == 0:
            ev_rest(w, 3)
        conv(l, M // CT // 2, M // CT)
        halo_fin(l)
        conv(l, 0, 1)
        stats_send(l)
        if more:
            ev_d(v + 3, 1)
        activate(l)
        for yo in range(Y):
            for j in range(Z):
                if yo > 0 and not scheme_a[w]:
                    wait_w(w, zorder(j) * Y + wrap(y + yo, Y))
                do_chunk(l, j, yo)
        flush_chunk()
        if more:
            ev_d(v + 3, 2)
            send_own(w + 3)
            ev_rest(v + 3, 3)
            ev_d(g + 3, 1)
        finish(l)
        if more:
            ev_d(g + 3, 2)
            norm_send(l + 1)
            ev_rest(g + 3, 3)
            ev_d(w + 3, 1)
            tok_relay(l + 1)
            ev_rest(w + 3, 2)
    drain()


def solution(mesh):
    sp, tp = mesh.shape["sp"], mesh.shape["tp"]
    Y = 1
    while (2 * Y) * (2 * Y) <= sp:
        Y *= 2
    Z, X = sp // Y, tp // 2

    def body(*args):
        hidden, norm_gain, w_value, w_gate, conv_weight, conv_bias, chan_gain, chan_shift, w_out = args
        own_rows, D = hidden.shape
        L, rows, C = w_value.shape
        wcols = w_out.shape[2]
        M = own_rows * tp
        U = 3 * L
        vm = pltpu.VMEM
        dma = pltpu.SemaphoreType.DMA
        nx = max(X - 1, 1)
        return pl.pallas_call(
            functools.partial(kernel, Z, Y, X),
            out_shape=jax.ShapeDtypeStruct((own_rows, D), BF16),
            in_specs=[pl.BlockSpec(memory_space=pltpu.VMEM)] * 9,
            out_specs=pl.BlockSpec(memory_space=pltpu.VMEM),
            scratch_shapes=[
                vm((L, sp * rows, C), BF16), vm((L, sp * rows, C), BF16), vm((L, sp, C, wcols), BF16),
                vm((L, M, D), BF16),
                vm((L, sp, 2 * X, own_rows, wcols), BF16), vm((L, sp, X, own_rows, wcols), BF16),
                vm((L, sp, nx, own_rows, wcols), BF16), vm((L, sp, nx, own_rows, wcols), BF16),
                vm((C // LANES, HALO + M, LANES), F32), vm((L, 2, HALO, C), BF16),
                vm((M, C), F32), vm((M, LANES), F32), vm((M, LANES), F32),
                vm((L, tp, 8, M), F32), vm((M, C), BF16), vm((own_rows, D), BF16),
                dma((U, sp)), dma((U, sp)), dma((U, Y)), dma((U, Z, max(Y - 1, 1))),
                dma((L, 2 * X)), dma((L, tp)), dma((L,)), dma((L,)), dma((L, tp - 1)), dma((L, tp - 1)),
                dma((L, sp)), dma((L, sp)), dma((L, sp, nx)), dma((L, sp, nx)),
            ],
            compiler_params=pltpu.CompilerParams(
                collective_id=0, has_side_effects=True, vmem_limit_bytes=65000 * 1024),
        )(*args)

    placed = (
        P(("sp", "tp"), None), P(), P(None, "sp", "tp"), P(None, "sp", "tp"), P(None, None, "tp"),
        P(None, "tp"), P(None, "tp"), P(None, "tp"), P(None, "tp", "sp"),
    )
    return jax.shard_map(
        body, mesh=mesh, in_specs=placed, out_specs=P(("sp", "tp"), None), check_vma=False)
```
